32 devices in a mesh: ra: 4 (over z), cb: 4 (over y, x), dp: 2 (over core).
Axes of the slice: x: 2, y: 2, z: 4, core: 2. Of those that a mesh axis runs over, the one named last changes fastest.
Arguments:
- tokens: bfloat16 [1024, 4096], P('dp', 'ra'), may hold values from -160 to 160, as said below
- first_gain: bfloat16 [4096], P('ra'), may hold values from 0.099609375 to 1.8984375
- first_gate: bfloat16 [4096, 6144], P('ra', 'cb'), may hold values from -0.125 to 0.125
- first_up: bfloat16 [4096, 6144], P('ra', 'cb'), may hold values from -0.125 to 0.125
- first_down: bfloat16 [6144, 4096], P(('cb', 'ra')), may hold values from -0.109375 to 0.109375
- first_branch: bfloat16 [4096], P('ra'), may hold values from 1 to 4
- second_gain: bfloat16 [4096], P('ra'), may hold values from 0.099609375 to 1.8984375
- second_gate: bfloat16 [4096, 6144], P('ra', 'cb'), may hold values from -0.125 to 0.125
- second_up: bfloat16 [4096, 6144], P('ra', 'cb'), may hold values from -0.125 to 0.125
- second_down: bfloat16 [6144, 4096], P(('cb', 'ra')), may hold values from -0.109375 to 0.109375
- second_branch: bfloat16 [4096], P('ra'), may hold values from 1 to 4
Outputs:
- mixed_out: bfloat16 [1024, 4096], P('dp', 'ra')
The draws below stay inside these ranges and needn't reach their ends.
Inputs may be any that keep to these rules, and one draw needn't show every extreme that they name: `tokens`: activations whose scale varies by token and by feature.
All inputs are finite; a program needn't handle non-finite values.
Results may differ from the reference program's by a relative error of at most 0.035.
Values may be sent and summed in bfloat16 or wider, within the bound.
A program may use at most 64 MiB of HBM per device.

```python
import math
import jax
import jax.numpy as jnp
from jax import lax

D = 4096
FF = 6144
TOKENS = 1024


def draw_tokens(key, part):
    first_key, second_key, third_key = jax.random.split(jax.random.fold_in(key, 11), 3)
    columns = jnp.exp(jnp.log(6.0) * jnp.arange(D, dtype=jnp.float32) / D) * jax.random.uniform(second_key, (D,), jnp.float32, 0.5, 1.5)
    rows = jnp.exp(jax.random.uniform(third_key, (TOKENS, 1), jnp.float32, 0.0, jnp.log(4.0)))
    base = jax.random.truncated_normal(first_key, -4.0, 4.0, (TOKENS, D), jnp.float32)
    return (base * rows * columns[None, :]).astype(jnp.bfloat16)


def raised(array, rng, source, target, blocks, factor):
    def block_of(axis_at):
        return (jnp.arange(array.shape[axis_at]) // (array.shape[axis_at] // blocks)).reshape((-1,) + (1,) * (array.ndim - 1 - axis_at))

    first = jax.random.permutation(rng, blocks)[block_of(target)]
    second = (block_of(target) + blocks // 2) % blocks
    return jnp.where((block_of(source) == first) | (block_of(source) == second), factor * array, array)


def steps_of(key, shape, pieces, smallest, top_value):
    loudness = 1.0
    for dim, parts in pieces:
        draws = jax.random.uniform(jax.random.fold_in(jax.random.fold_in(key, 6), dim), (parts,), jnp.float32, smallest / len(pieces), top_value / len(pieces))
        loudness = loudness * jnp.repeat(jnp.exp(draws), shape[dim] // parts).reshape((-1,) + (1,) * (len(shape) - 1 - dim))
    return loudness


def gaussian_with(key, dims, scale, reach, shards, heavy, kind=jnp.bfloat16):
    values = scale * jax.random.normal(key, dims, jnp.float32)
    if shards:
        values = values * steps_of(key, dims, shards, -0.22, 0.18)
    return jnp.clip(raised(values, jax.random.fold_in(key, 3), *heavy), -reach, reach).astype(kind)


def setup_inputs(seed: int = 0) -> dict:
    key_of = jax.random.split(jax.random.key(seed), 12)
    return {
        "tokens": draw_tokens(jax.random.fold_in(key_of[11], 71), 0),
        "first_gain": jnp.clip(1.0 + 0.18 * jax.random.normal(key_of[1], (D,), jnp.float32), 0.099609375, 1.8984375).astype(jnp.bfloat16),
        "first_gate": gaussian_with(key_of[2], (D, FF), D ** -0.5, 0.125, ((0, 4), (1, 4)), (0, 1, 4, 2.0)),
        "first_up": gaussian_with(key_of[3], (D, FF), D ** -0.5, 0.125, ((0, 4), (1, 4)), (0, 1, 4, 2.0)),
        "first_down": gaussian_with(key_of[4], (FF, D), FF ** -0.5, 0.109375, ((0, 16),), (0, 1, 16, 2.0)),
        "first_branch": jnp.clip(jnp.exp(math.log(4.0) - 1.3862944 * jax.random.uniform(key_of[5], (D,), jnp.float32) ** steps_of(key_of[5], (D,), ((0, 4),), -0.2, 0.2)), 1.0, 4.0).astype(jnp.bfloat16),
        "second_gain": jnp.clip(1.0 + 0.18 * jax.random.normal(key_of[6], (D,), jnp.float32), 0.099609375, 1.8984375).astype(jnp.bfloat16),
        "second_gate": gaussian_with(key_of[7], (D, FF), D ** -0.5, 0.125, ((0, 4), (1, 4)), (0, 1, 4, 2.0)),
        "second_up": gaussian_with(key_of[8], (D, FF), D ** -0.5, 0.125, ((0, 4), (1, 4)), (0, 1, 4, 2.0)),
        "second_down": gaussian_with(key_of[9], (FF, D), FF ** -0.5, 0.109375, ((0, 16),), (0, 1, 16, 2.0)),
        "second_branch": jnp.clip(jnp.exp(math.log(4.0) - 1.3862944 * jax.random.uniform(key_of[10], (D,), jnp.float32) ** steps_of(key_of[10], (D,), ((0, 4),), -0.2, 0.2)), 1.0, 4.0).astype(jnp.bfloat16),
    }


epsilon = 1e-06
residual_scale = 0.25

def half_step(values, norm_gain, w_gate, w_up, w_down, branch_gain):
    wide_values = values.astype(jnp.float32)
    mean_square = lax.optimization_barrier(jnp.mean(wide_values * wide_values, axis=1, keepdims=True))
    normed = (wide_values * lax.rsqrt(mean_square + epsilon) * norm_gain.astype(jnp.float32)).astype(jnp.bfloat16)
    gate = jnp.dot(normed, w_gate, preferred_element_type=jnp.float32)
    upward = jnp.dot(normed, w_up, preferred_element_type=jnp.float32)
    hidden = (jax.nn.silu(gate) * upward).astype(jnp.bfloat16)
    branch = jnp.dot(hidden, w_down, preferred_element_type=jnp.float32)
    return (residual_scale * wide_values + 0.5 * branch_gain.astype(jnp.float32) * branch).astype(jnp.bfloat16)

def reference(tokens, first_gain, first_gate, first_up, first_down, first_branch, second_gain, second_gate, second_up, second_down, second_branch):
    middle = half_step(tokens, first_gain, first_gate, first_up, first_down, first_branch)
    return half_step(middle, second_gain, second_gate, second_up, second_down, second_branch)
```

```python
import functools

import jax
import jax.numpy as jnp
from jax import lax
from jax.experimental import pallas as pl
from jax.experimental.pallas import tpu as pltpu
from jax.sharding import PartitionSpec as P

epsilon = 1e-06
residual_scale = 0.25
MESH = pl.DeviceIdType.MESH
CHUNKS = 4


def half_step(values, norm_gain, w_gate, w_up, w_down, branch_gain):
    wide_values = values.astype(jnp.float32)
    width = values.shape[1] * lax.axis_size("ra")
    squares = lax.psum(jnp.sum(wide_values * wide_values, axis=1), "ra")
    scale = lax.rsqrt(squares / width + epsilon)
    normed = (wide_values * scale[:, None] * norm_gain.astype(jnp.float32)).astype(jnp.bfloat16)
    gate_part = jnp.dot(normed, w_gate, preferred_element_type=jnp.float32)
    up_part = jnp.dot(normed, w_up, preferred_element_type=jnp.float32)
    gate, upward = (
        lax.psum_scatter(
            gate_part.astype(jnp.bfloat16), "ra", scatter_dimension=1, tiled=True
        ).astype(jnp.float32),
        lax.psum_scatter(
            up_part.astype(jnp.bfloat16), "ra", scatter_dimension=1, tiled=True
        ).astype(jnp.float32),
    )
    hidden = (jax.nn.silu(gate) * upward).astype(jnp.bfloat16)
    terms = jnp.dot(hidden, w_down, preferred_element_type=jnp.float32)
    partial_value = lax.psum_scatter(
        terms.astype(jnp.bfloat16), "ra", scatter_dimension=1, tiled=True
    )
    branch = lax.psum(partial_value, "cb").astype(jnp.float32)
    return (residual_scale * wide_values + 0.5 * branch_gain.astype(jnp.float32) * branch).astype(
        jnp.bfloat16
    )


def plain(
    tokens,
    first_gain,
    first_gate,
    first_up,
    first_down,
    first_branch,
    second_gain,
    second_gate,
    second_up,
    second_down,
    second_branch,
):
    middle = half_step(tokens, first_gain, first_gate, first_up, first_down, first_branch)
    return half_step(middle, second_gain, second_gate, second_up, second_down, second_branch)


def kernel(
    n, m, K, rows, wide, hid,
    tok, gate0, up0, down0, gate1, up1, down1, gains, branches, out,
    wgu, wd, xbuf, xg, part, recv_a, yst, recv_y, sst, recv_s, acc, ytot, ownz, sq, recv_q,
    w_sem, d_sem, x_sem, o_sem,
    as_sem, ar_sem, ys_sem, yr_sem, ss_sem, sr_sem, gs_sem, gr_sem, qs_sem, qr_sem,
):
    r = lax.axis_index("ra")
    c = lax.axis_index("cb")
    T = rows // K
    q = wide // m
    full = n * wide
    S = 2 * K
    f32 = jnp.float32

    def w_copies(h):
        gate, up = ((gate0, up0), (gate1, up1))[h]
        made = []
        for d in range(n):
            for i, src in enumerate((gate, up)):
                made.append(pltpu.make_async_copy(
                    src.at[:, pl.ds(d * hid, hid)],
                    wgu.at[h, d, :, pl.ds(i * hid, hid)],
                    w_sem.at[h, d, i],
                ))
        return made

    def d_copies(h):
        down = (down0, down1)[h]
        return [
            pltpu.make_async_copy(
                down.at[:, pl.ds(z * wide + p * q, q)],
                wd.at[h, p, :, pl.ds(z * q, q)],
                d_sem.at[h, p, z],
            )
            for p in range(m)
            for z in range(n)
        ]

    x_copies = [
        pltpu.make_async_copy(tok.at[:, pl.ds(p * q, q)], xbuf.at[0, p], x_sem.at[p])
        for p in range(m)
    ]
    for copy in x_copies + w_copies(0) + d_copies(0) + w_copies(1) + d_copies(1):
        copy.start()

    barrier = pltpu.get_barrier_semaphore()
    for o in range(1, n):
        pl.semaphore_signal(barrier, inc=1, device_id={"ra": lax.rem(r + o, n)}, device_id_type=MESH)
    for o in range(1, m):
        pl.semaphore_signal(barrier, inc=1, device_id={"cb": lax.rem(c + o, m)}, device_id_type=MESH)

    def rows_of(k):
        return pl.ds(pl.multiple_of(k * T, T), T)

    def a_copy(s, d, target, slot):
        h, k = s // K, s % K
        return pltpu.make_async_remote_copy(
            src_ref=part.at[d, rows_of(k)],
            dst_ref=recv_a.at[h, slot, rows_of(k)],
            send_sem=as_sem.at[k, d],
            recv_sem=ar_sem.at[s, slot],
            device_id={"ra": target},
            device_id_type=MESH,
        )

    def y_copy(s, dest, src):
        h, k = s // K, s % K
        return pltpu.make_async_remote_copy(
            src_ref=yst.at[dest, rows_of(k)],
            dst_ref=recv_y.at[h, src, rows_of(k)],
            send_sem=ys_sem.at[k, dest],
            recv_sem=yr_sem.at[s, src],
            device_id={"cb": dest},
            device_id_type=MESH,
        )

    def s_copy(s, dest, src):
        h, k = s // K, s % K
        return pltpu.make_async_remote_copy(
            src_ref=sst.at[dest, rows_of(k)],
            dst_ref=recv_s.at[h, src, rows_of(k)],
            send_sem=ss_sem.at[k, dest],
            recv_sem=sr_sem.at[s, src],
            device_id={"ra": dest},
            device_id_type=MESH,
        )

    def g_copy(s, dest, src):
        h, k = s // K, s % K
        return pltpu.make_async_remote_copy(
            src_ref=xbuf.at[h + 1, src, rows_of(k)],
            dst_ref=xbuf.at[h + 1, src, rows_of(k)],
            send_sem=gs_sem.at[s, dest],
            recv_sem=gr_sem.at[s, src],
            device_id={"cb": dest},
            device_id_type=MESH,
        )

    def q_copy(s, dest, src):
        return pltpu.make_async_remote_copy(
            src_ref=sq.at[s],
            dst_ref=recv_q.at[s, src],
            send_sem=qs_sem.at[s, dest],
            recv_sem=qr_sem.at[s, src],
            device_id={"ra": dest},
            device_id_type=MESH,
        )

    def send_part(s, d, value, target, slot):
        k = s % K

        @pl.when(s >= K)
        def _():
            a_copy(s, d, target, slot).wait_send()

        part[d, rows_of(k), :] = value.astype(jnp.bfloat16)
        a_copy(s, d, target, slot).start()

    def ahead(s):
        h, k = s // K, s % K
        total = jnp.zeros((T, 128), f32)
        for p in range(m):
            x = xbuf[h, p, rows_of(k), :].astype(f32)
            xg[rows_of(k), p * q:(p + 1) * q] = (x * gains[h, :, p * q:(p + 1) * q]).astype(jnp.bfloat16)
            x2 = x * x
            for i in range(q // 128):
                total = total + x2[:, i * 128:(i + 1) * 128]
        column = jnp.sum(total, axis=1, keepdims=True)
        sq[s] = jnp.transpose(jnp.broadcast_to(column, (T, 128)))[:8]

        def q_send(o, carry):
            q_copy(s, lax.rem(r + o, n), r).start()
            return carry

        lax.fori_loop(1, n, q_send, 0)

        @pl.when(jnp.logical_or(r == 0, r == n - 1))
        def _():
            def head(j, carry):
                d = jnp.where(r == 0, n - 1 - j, j)
                target = jnp.where(r == 0, 1, n - 2)
                slot = jnp.where(r == 0, d + 1, d)
                value = jnp.dot(xg[rows_of(k), :], wgu[h, d], preferred_element_type=f32)
                send_part(s, d, value, target, slot)
                return carry

            lax.fori_loop(0, n - 1, head, 0)

    def forward(s, leftward):
        h, k = s // K, s % K

        def step(j, carry):
            d = jnp.where(leftward, j, n - 1 - j)
            target = jnp.where(leftward, r - 1, r + 1)
            slot = jnp.where(leftward, d, d + 1)

            @pl.when(jnp.where(leftward, d < r, d > r))
            def _():
                acc[...] = jnp.dot(xg[rows_of(k), :], wgu[h, d], preferred_element_type=f32)
                a_copy(s, d, target, slot).wait_recv()
                send_part(s, d, acc[...] + recv_a[h, slot, rows_of(k), :].astype(f32), target, slot)

            return carry

        @pl.when(jnp.logical_and(r > 0, r < n - 1))
        def _():
            lax.fori_loop(0, n - 1, step, 0)

    near_left = r >= n // 2
    far_left = r < n // 2

    def finish(s):
        h, k = s // K, s % K
        acc[...] = jnp.dot(xg[rows_of(k), :], wgu[h, r], preferred_element_type=f32)

        def q_wait(o, carry):
            src = lax.rem(r + o, n)
            q_copy(s, src, src).wait_recv()
            return carry + recv_q[s, src]

        squares = lax.fori_loop(1, n, q_wait, sq[s])
        scale_row = lax.rsqrt(squares / full + epsilon)
        scale = jnp.transpose(jnp.broadcast_to(scale_row[:1], (128, T)))[:, :1]

        @pl.when(r > 0)
        def _():
            a_copy(s, r, r, r + 1).wait_recv()
            acc[...] += recv_a[h, r + 1, rows_of(k), :].astype(f32)

        @pl.when(r < n - 1)
        def _():
            a_copy(s, r, r, r).wait_recv()
            acc[...] += recv_a[h, r, rows_of(k), :].astype(f32)

        gate = acc[:, :hid] * scale
        upward = acc[:, hid:] * scale
        hidden = (gate / (1.0 + jnp.exp(-gate)) * upward).astype(jnp.bfloat16)

        def down(o, carry):
            dest = lax.rem(c + o, m)
            value = jnp.dot(hidden, wd[h, dest], preferred_element_type=f32)

            @pl.when(s >= K)
            def _():
                y_copy(s, dest, c).wait_send()

            yst[dest, rows_of(k), :] = value.astype(jnp.bfloat16)
            y_copy(s, dest, c).start()
            return carry

        lax.fori_loop(1, m, down, 0)
        ytot[...] = jnp.dot(hidden, wd[h, c], preferred_element_type=f32)

    def plane(s):
        h, k = s // K, s % K

        def add(o, carry):
            src = lax.rem(c + o, m)
            y_copy(s, src, src).wait_recv()
            ytot[...] += recv_y[h, src, rows_of(k), :].astype(f32)
            return carry

        lax.fori_loop(1, m, add, 0)

        def send(o, carry):
            dest = lax.rem(r + o, n)

            @pl.when(s >= K)
            def _():
                s_copy(s, dest, r).wait_send()

            sst[dest, rows_of(k), :] = ytot[:, pl.ds(pl.multiple_of(dest * q, q), q)].astype(jnp.bfloat16)
            s_copy(s, dest, r).start()
            return carry

        lax.fori_loop(1, n, send, 0)
        ownz[rows_of(k), :] = ytot[:, pl.ds(pl.multiple_of(r * q, q), q)]

    def gather(s):
        h, k = s // K, s % K

        def add(o, carry):
            src = lax.rem(r + o, n)
            s_copy(s, src, src).wait_recv()
            ownz[rows_of(k), :] += recv_s[h, src, rows_of(k), :].astype(f32)
            return carry

        lax.fori_loop(1, n, add, 0)
        gain = branches[h, :, pl.ds(pl.multiple_of(c * q, q), q)]
        x = xbuf[h, c, rows_of(k), :].astype(f32)
        xbuf[h + 1, c, rows_of(k), :] = (
            residual_scale * x + 0.5 * gain * ownz[rows_of(k), :]
        ).astype(jnp.bfloat16)

        def send(o, carry):
            g_copy(s, lax.rem(c + o, m), c).start()
            return carry

        lax.fori_loop(1, m, send, 0)

    def o_copy(k, p):
        return pltpu.make_async_copy(
            xbuf.at[2, p, rows_of(k)], out.at[rows_of(k), pl.ds(p * q, q)], o_sem.at[k, p]
        )

    def arrive(s):
        k = s % K

        def wait(o, carry):
            src = lax.rem(c + o, m)
            g_copy(s, src, src).wait_recv()
            return carry

        lax.fori_loop(1, m, wait, 0)

        @pl.when(s >= K)
        def _():
            for p in range(m):
                o_copy(k, p).start()

    for copy in x_copies + w_copies(0):
        copy.wait()
    pl.semaphore_wait(barrier, n + m - 2)
    ahead(jnp.int32(0))
    forward(jnp.int32(0), near_left)
    for copy in d_copies(0):
        copy.wait()

    def slot_body(t, carry):
        @pl.when(t == K - 1)
        def _():
            for copy in w_copies(1) + d_copies(1):
                copy.wait()

        @pl.when(jnp.logical_and(t >= 3, t < S + 3))
        def _():
            arrive(t - 3)

        @pl.when(t + 1 < S)
        def _():
            ahead(t + 1)

        @pl.when(t < S)
        def _():
            forward(t, far_left)

        @pl.when(jnp.logical_and(t >= 2, t < S + 2))
        def _():
            gather(t - 2)

        @pl.when(jnp.logical_and(t >= 1, t < S + 1))
        def _():
            plane(t - 1)

        @pl.when(t < S)
        def _():
            finish(t)

        @pl.when(t + 1 < S)
        def _():
            forward(t + 1, near_left)

        return carry

    lax.fori_loop(0, S + 3, slot_body, 0)

    def drain(k, carry):
        def over_ra(o, inner):
            dest = lax.rem(r + o, n)
            a_copy(k, dest, dest, dest).wait_send()
            s_copy(k, dest, r).wait_send()
            q_copy(k, dest, r).wait_send()
            q_copy(k + K, dest, r).wait_send()
            return inner

        def over_cb(o, inner):
            dest = lax.rem(c + o, m)
            y_copy(k, dest, c).wait_send()
            g_copy(k, dest, c).wait_send()
            g_copy(k + K, dest, c).wait_send()
            return inner

        lax.fori_loop(1, n, over_ra, 0)
        lax.fori_loop(1, m, over_cb, 0)
        for p in range(m):
            o_copy(k, p).wait()
        return carry

    lax.fori_loop(0, K, drain, 0)


def fused(
    tokens,
    first_gain,
    first_gate,
    first_up,
    first_down,
    first_branch,
    second_gain,
    second_gate,
    second_up,
    second_down,
    second_branch,
):
    n, m = lax.axis_size("ra"), lax.axis_size("cb")
    rows, wide = tokens.shape
    hid = first_down.shape[0]
    K = CHUNKS
    S = 2 * K
    T = rows // K
    q = wide // m
    f32, bf16 = jnp.float32, jnp.bfloat16
    gains = jnp.stack([first_gain, second_gain]).astype(f32).reshape(2, 1, wide)
    branches = jnp.stack([first_branch, second_branch]).astype(f32).reshape(2, 1, wide)
    dma = pltpu.SemaphoreType.DMA
    anywhere = pl.BlockSpec(memory_space=pl.ANY)
    inside = pl.BlockSpec(memory_space=pltpu.VMEM)
    return pl.pallas_call(
        functools.partial(kernel, n, m, K, rows, wide, hid),
        out_shape=jax.ShapeDtypeStruct((rows, wide), bf16),
        in_specs=[anywhere] * 7 + [inside] * 2,
        out_specs=anywhere,
        scratch_shapes=[
            pltpu.VMEM((2, n, wide, 2 * hid), bf16),
            pltpu.VMEM((2, m, hid, n * q), bf16),
            pltpu.VMEM((3, m, rows, q), bf16),
            pltpu.VMEM((rows, wide), bf16),
            pltpu.VMEM((n, rows, 2 * hid), bf16),
            pltpu.VMEM((2, n + 1, rows, 2 * hid), bf16),
            pltpu.VMEM((m, rows, n * q), bf16),
            pltpu.VMEM((2, m, rows, n * q), bf16),
            pltpu.VMEM((n, rows, q), bf16),
            pltpu.VMEM((2, n, rows, q), bf16),
            pltpu.VMEM((T, 2 * hid), f32),
            pltpu.VMEM((T, n * q), f32),
            pltpu.VMEM((rows, q), f32),
            pltpu.VMEM((S, 8, T), f32),
            pltpu.VMEM((S, n, 8, T), f32),
            dma((2, n, 2)),
            dma((2, m, n)),
            dma((m,)),
            dma((K, m)),
            dma((K, n)),
            dma((S, n + 1)),
            dma((K, m)),
            dma((S, m)),
            dma((K, n)),
            dma((S, n)),
            dma((S, m)),
            dma((S, m)),
            dma((S, n)),
            dma((S, n)),
        ],
        compiler_params=pltpu.CompilerParams(
            collective_id=0, has_side_effects=True, vmem_limit_bytes=66000000
        ),
        name="ffn_pair",
    )(
        tokens, first_gate, first_up, first_down, second_gate, second_up, second_down,
        gains, branches,
    )


def shards(*arrays):
    n, m = lax.axis_size("ra"), lax.axis_size("cb")
    rows, wide = arrays[0].shape
    hid = arrays[4].shape[0]
    even = rows % (128 * CHUNKS) == 0 and hid % 128 == 0 and wide % (128 * m) == 0
    return fused(*arrays) if even and n > 1 and m > 1 else plain(*arrays)


def solution(mesh):
    return jax.shard_map(
        shards,
        mesh=mesh,
        in_specs=(
            P("dp", "ra"),
            P("ra"),
            P("ra", "cb"),
            P("ra", "cb"),
            P(("cb", "ra"), None),
            P("ra"),
            P("ra"),
            P("ra", "cb"),
            P("ra", "cb"),
            P(("cb", "ra"), None),
            P("ra"),
        ),
        out_specs=P("dp", "ra"),
        check_vma=False,
    )
```
